32 devices in a mesh: fs: 8 (over z, x), tp: 4 (over y, core).
Axes of the slice: x: 2, y: 2, z: 4, core: 2. Of those that a mesh axis runs over, the one named last changes fastest.
Arguments:
- later_in: bfloat16 [8192, 2048], P('fs'), may hold values from -3 to 3
- earlier_in: bfloat16 [8192, 2048], P('fs'), may hold values from -3 to 3
- cotangent: bfloat16 [8192, 2048], P('fs'), may hold values from -6 to 6
- gate_weight: bfloat16 [2048, 5632], P('fs', 'tp'), may hold values from -0.125 to 0.125
- up_weight: bfloat16 [2048, 5632], P('fs', 'tp'), may hold values from -0.125 to 0.125
- down_weight: bfloat16 [2048, 5632], P('fs', 'tp'), may hold values from -0.078125 to 0.078125
- norm_gain: bfloat16 [2048], replicated, may hold values from 0.099609375 to 1.8984375
- gate_sum: float32 [2048, 5632], P('fs', 'tp'), may hold values from -96 to 96
- up_sum: float32 [2048, 5632], P('fs', 'tp'), may hold values from -96 to 96
- down_sum: float32 [2048, 5632], P('fs', 'tp'), may hold values from -96 to 96
- gain_sum: float32 [2048], replicated, may hold values from -192 to 192
Outputs:
- later_out: bfloat16 [8192, 2048], P(('fs', 'tp'))
- later_hidden: bfloat16 [8192, 5632], P('fs', 'tp')
- earlier_grad: bfloat16 [8192, 2048], P(('fs', 'tp'))
- gate_sum_new: float32 [2048, 5632], P('fs', 'tp')
- up_sum_new: float32 [2048, 5632], P('fs', 'tp')
- down_sum_new: float32 [2048, 5632], P('fs', 'tp')
- gain_sum_new: float32 [2048], replicated
The draws below stay inside these ranges and needn't reach their ends.
All inputs are finite; a program needn't handle non-finite values.
Results may differ from the reference program's by a relative error of at most 0.013.
Values may be sent and summed in bfloat16 or wider, within the bound.
A program may use at most 128 MiB of HBM per device.

```python
import jax
import jax.numpy as jnp
from jax import lax

D = 2048
FF = 5632
TOKENS = 8192
N_TP = 4


def raised(array, stream_key, source, target, blocks, factor):
    owner, partner = [(jnp.arange(array.shape[position]) // (array.shape[position] // blocks)).reshape([-1 if axis == position else 1 for axis in range(array.ndim)]) for position in (source, target)]
    chosen = jax.random.permutation(stream_key, blocks)[partner]
    strong = (owner == chosen) | (owner == (partner + blocks // 2) % blocks)
    return jnp.where(strong, factor * array, array)


def steps_of(own_key, shape, pieces, least, high):
    def one(axis_at, blocks):
        steps = jax.random.uniform(jax.random.fold_in(jax.random.fold_in(own_key, 6), axis_at), (blocks,), jnp.float32, least / len(pieces), high / len(pieces))
        return jnp.repeat(jnp.exp(steps), shape[axis_at] // blocks).reshape((-1,) + (1,) * (len(shape) - axis_at - 1))

    factor_of = one(*pieces[0])
    for cut in pieces[1:]:
        factor_of = factor_of * one(*cut)
    return factor_of


def centred(own_key, extent, spread, bound, cuts=(), dtype=jnp.bfloat16):
    drawn = spread * jax.random.normal(own_key, extent, jnp.float32)
    if cuts:
        drawn = drawn * steps_of(own_key, extent, cuts, -0.22, 0.18)
    return jnp.clip(drawn, -bound, bound).astype(dtype)


def bell_draw_with(stream_key, shape, scale, bound, shards, heavy, kind=jnp.bfloat16):
    array = scale * jax.random.normal(stream_key, shape, jnp.float32)
    if shards:
        array = array * steps_of(stream_key, shape, shards, -0.22, 0.18)
    return jnp.clip(raised(array, jax.random.fold_in(stream_key, 3), *heavy), -bound, bound).astype(kind)


def setup_inputs(seed: int = 0) -> dict:
    streams_of = jax.random.split(jax.random.key(seed), 12)
    return {
        "later_in": centred(streams_of[0], (TOKENS, D), 0.5, 3.0, ((0, 8),)),
        "earlier_in": centred(streams_of[1], (TOKENS, D), 0.5, 3.0, ((0, 8),)),
        "cotangent": bell_draw_with(streams_of[2], (TOKENS, D), 1.0, 6.0, ((0, 8),), (0, 1, 8, 2.0)),
        "gate_weight": centred(streams_of[3], (D, FF), D ** -0.5, 0.125, ((0, 8), (1, 4))),
        "up_weight": centred(streams_of[4], (D, FF), D ** -0.5, 0.125, ((0, 8), (1, 4))),
        "down_weight": centred(streams_of[5], (D, FF), FF ** -0.5, 0.078125, ((0, 8), (1, 4))),
        "norm_gain": jnp.clip(1.0 + 0.18 * jax.random.normal(streams_of[6], (D,), jnp.float32), 0.099609375, 1.8984375).astype(jnp.bfloat16),
        "gate_sum": centred(streams_of[7], (D, FF), 16.0, 96.0, ((0, 8), (1, 4)), jnp.float32),
        "up_sum": centred(streams_of[8], (D, FF), 16.0, 96.0, ((0, 8), (1, 4)), jnp.float32),
        "down_sum": centred(streams_of[9], (D, FF), 16.0, 96.0, ((0, 8), (1, 4)), jnp.float32),
        "gain_sum": centred(streams_of[10], (D,), 32.0, 192.0, (), jnp.float32),
    }


norm_floor = 0.05

def normalize(tokens_in, norm_gain):
    values = tokens_in.astype(jnp.float32)
    row_scale = jax.lax.rsqrt(lax.optimization_barrier(jnp.mean(values * values, axis=1, keepdims=True)) + norm_floor)
    unit_rows = values * row_scale
    normed = (unit_rows * norm_gain.astype(jnp.float32)).astype(jnp.bfloat16)
    return (row_scale, unit_rows, normed)

def rounded(partial_value):
    return jax.lax.optimization_barrier(partial_value.astype(jnp.bfloat16)).astype(jnp.float32)

def reference(later_in, earlier_in, cotangent, gate_weight, up_weight, down_weight, norm_gain, gate_sum, up_sum, down_sum, gain_sum):
    block_width = FF // N_TP
    gain_f = norm_gain.astype(jnp.float32)
    normed_later = normalize(later_in, norm_gain)[2]
    gate_later = jnp.dot(normed_later, gate_weight, preferred_element_type=jnp.float32)
    up_later = jnp.dot(normed_later, up_weight, preferred_element_type=jnp.float32)
    later_hidden = (jax.nn.silu(gate_later) * up_later).astype(jnp.bfloat16)
    branch_total = jnp.zeros(later_in.shape, jnp.float32)
    for block_index in range(N_TP):
        first = block_index * block_width
        partial_value = jnp.dot(later_hidden[:, first:first + block_width], down_weight[:, first:first + block_width].T, preferred_element_type=jnp.float32)
        branch_total = branch_total + rounded(partial_value)
    later_out = (later_in.astype(jnp.float32) + 0.5 * branch_total).astype(jnp.bfloat16)
    row_scale, unit_rows, normed = normalize(earlier_in, norm_gain)
    gate_pre = jnp.dot(normed, gate_weight, preferred_element_type=jnp.float32)
    up_pre = jnp.dot(normed, up_weight, preferred_element_type=jnp.float32)
    sigmoid_gate = jax.nn.sigmoid(gate_pre)
    activated = gate_pre * sigmoid_gate
    hidden_earlier = (activated * up_pre).astype(jnp.bfloat16)
    dhidden = jnp.dot(cotangent, down_weight, preferred_element_type=jnp.float32)
    dgate = (0.5 * dhidden * up_pre * sigmoid_gate * (1.0 + gate_pre * (1.0 - sigmoid_gate))).astype(jnp.bfloat16)
    dupper = (0.5 * dhidden * activated).astype(jnp.bfloat16)
    grad_total = jnp.zeros(earlier_in.shape, jnp.float32)
    dnormed_total = jnp.zeros(earlier_in.shape, jnp.float32)
    for block_index in range(N_TP):
        first = block_index * block_width
        dnormed_part = jnp.dot(dgate[:, first:first + block_width], gate_weight[:, first:first + block_width].T, preferred_element_type=jnp.float32) + jnp.dot(dupper[:, first:first + block_width], up_weight[:, first:first + block_width].T, preferred_element_type=jnp.float32)
        dnormed_total = dnormed_total + dnormed_part
        weighted = dnormed_part * gain_f
        branch_part = row_scale * (weighted - unit_rows * lax.optimization_barrier(jnp.mean(weighted * unit_rows, axis=1, keepdims=True)))
        grad_total = grad_total + rounded(branch_part)
    earlier_grad = (cotangent.astype(jnp.float32) + grad_total).astype(jnp.bfloat16)
    gate_sum_new = gate_sum + jnp.dot(normed.T, dgate, preferred_element_type=jnp.float32)
    up_sum_new = up_sum + jnp.dot(normed.T, dupper, preferred_element_type=jnp.float32)
    down_sum_new = down_sum + 0.5 * jnp.dot(cotangent.T, hidden_earlier, preferred_element_type=jnp.float32)
    gain_sum_new = gain_sum + lax.optimization_barrier(jnp.sum(dnormed_total * unit_rows, axis=0))
    return (later_out, later_hidden, earlier_grad, gate_sum_new, up_sum_new, down_sum_new, gain_sum_new)
```

```python
import jax
import jax.numpy as jnp
from jax import lax
from jax.sharding import PartitionSpec as P

norm_floor = 0.05


def normalize(tokens_in, norm_gain):
    values = tokens_in.astype(jnp.float32)
    row_scale = lax.rsqrt(jnp.mean(values * values, axis=1, keepdims=True) + norm_floor)
    unit_rows = values * row_scale
    normed = (unit_rows * norm_gain.astype(jnp.float32)).astype(jnp.bfloat16)
    return (row_scale, unit_rows, normed)


def transposed(matrix_a, matrix_b):
    return lax.dot_general(
        matrix_a, matrix_b, (((1,), (1,)), ((), ())), preferred_element_type=jnp.float32
    )


def outer_sum(matrix_a, matrix_b):
    return lax.dot_general(
        matrix_a, matrix_b, (((0,), (0,)), ((), ())), preferred_element_type=jnp.float32
    )


def own_rows(tokens_in, own_count):
    return lax.dynamic_slice_in_dim(tokens_in, lax.axis_index("tp") * own_count, own_count, 0)


def factors(count):
    outer = 1
    while outer * outer < count:
        outer *= 2
    while count % outer:
        outer //= 2
    return (outer, count // outer)


class Line:
    def __init__(self, is_outer):
        self.count = lax.axis_size("fs")
        outer, inner = factors(self.count)
        index = lax.axis_index("fs")
        self.size = outer if is_outer else inner
        self.stride = inner if is_outer else 1
        self.position = index // inner if is_outer else lax.rem(index, inner)

    def send(self, piece, shift, first, last):
        pairs = []
        for index in range(self.count):
            member = index // self.stride % self.size
            if first <= member <= last:
                pairs.append((index, index + shift * self.stride))
        return lax.ppermute(piece, "fs", pairs)

    def swap(self, piece):
        pairs = []
        for index in range(self.count):
            member = index // self.stride % self.size
            pairs.append((index, index + (1 - 2 * member) * self.stride))
        return lax.ppermute(piece, "fs", pairs)

    def gather(self, block):
        size, position = self.size, self.position
        if size == 1:
            return [block]
        if size == 2:
            return [block, self.swap(block)]
        up, down = [block], [block]
        for step in range(1, size):
            up.append(self.send(up[-1], 1, step - 1, size - 2))
            down.append(self.send(down[-1], -1, 1, size - step))
        return [block] + [
            jnp.where(position + step < size, down[step], up[size - step])
            for step in range(1, size)
        ]

    def scatter_sum(self, part, dtype):
        size = self.size
        own = part(0).astype(jnp.float32)
        if size == 1:
            return own, []
        if size == 2:
            came = self.swap(part(1))
            return own + came.astype(jnp.float32), [came]

        def plus(piece, came):
            return (piece.astype(jnp.float32) + came.astype(jnp.float32)).astype(dtype)

        up = self.send(part(size - 1), 1, 0, 0)
        down = self.send(part(1), -1, size - 1, size - 1)
        early = [up, down]
        for step in range(size - 2, 0, -1):
            up = self.send(plus(part(step), up), 1, 0, size - 1 - step)
            down = self.send(plus(part(size - step), down), -1, step, size - 1)
        return own + up.astype(jnp.float32) + down.astype(jnp.float32), early


def gather_fs(piece, outer_first):
    outer, inner = Line(True), Line(False)
    rows, cols = piece.shape
    buffer = jnp.zeros((outer.size, inner.size, rows, cols), piece.dtype)

    def slot(line, member):
        return lax.rem(line.position + member, line.size)

    if outer_first:
        column = jnp.zeros((outer.size, rows, cols), piece.dtype)
        for member, block in enumerate(outer.gather(piece)):
            column = lax.dynamic_update_slice(column, block[None], (slot(outer, member), 0, 0))
        for member, block in enumerate(inner.gather(column)):
            buffer = lax.dynamic_update_slice(
                buffer, block[:, None], (0, slot(inner, member), 0, 0)
            )
    else:
        group = jnp.zeros((inner.size, rows, cols), piece.dtype)
        for member, block in enumerate(inner.gather(piece)):
            group = lax.dynamic_update_slice(group, block[None], (slot(inner, member), 0, 0))
        for member, block in enumerate(outer.gather(group)):
            buffer = lax.dynamic_update_slice(buffer, block[None], (slot(outer, member), 0, 0, 0))
    return buffer.reshape(-1, cols)


def scatter_fs(total, outer_first):
    outer, inner = Line(True), Line(False)
    rows = total.shape[0] // (outer.size * inner.size)
    blocks = total.reshape(outer.size, inner.size, rows, total.shape[1])
    lines = (outer, inner) if outer_first else (inner, outer)
    axis = 0 if outer_first else 1

    def part_of(source, line, dimension):
        def part(member):
            index = lax.rem(line.position + member, line.size)
            return lax.dynamic_index_in_dim(source, index, dimension, keepdims=False)

        return part

    summed, early = lines[0].scatter_sum(part_of(blocks, lines[0], axis), total.dtype)
    summed = summed.astype(total.dtype)
    return lines[1].scatter_sum(part_of(summed, lines[1], 0), total.dtype)[0], early


def sum_all(part):
    for name in ("tp", "fs"):
        count = lax.axis_size(name)
        if count & (count - 1):
            part = lax.psum(part, name)
            continue
        step = 1
        while step < count:
            part = part + lax.ppermute(part, name, [(i, i ^ step) for i in range(count)])
            step *= 2
    return part


def forward(later_in, norm_gain, weights):
    w_gate, w_up, w_down = weights
    normed = normalize(later_in, norm_gain)[2]
    gate_pre = jnp.dot(normed, w_gate, preferred_element_type=jnp.float32)
    up_pre = jnp.dot(normed, w_up, preferred_element_type=jnp.float32)
    hidden = (jax.nn.silu(gate_pre) * up_pre).astype(jnp.bfloat16)
    own_count = later_in.shape[0] // lax.axis_size("tp")
    summed = lax.psum_scatter(
        transposed(hidden, w_down).astype(jnp.bfloat16), "tp", scatter_dimension=0, tiled=True
    ).astype(jnp.float32)
    later_out = (own_rows(later_in, own_count).astype(jnp.float32) + 0.5 * summed).astype(
        jnp.bfloat16
    )
    return (later_out, hidden)


def local(
    later_in,
    earlier_in,
    cotangent,
    gate_weight,
    up_weight,
    down_weight,
    norm_gain,
    gate_sum,
    up_sum,
    down_sum,
    gain_sum,
):
    w_gate = gather_fs(gate_weight, False)
    w_up = gather_fs(up_weight, True)
    w_down = gather_fs(down_weight, False)
    row_scale, unit_rows, normed = normalize(earlier_in, norm_gain)
    gate_pre = jnp.dot(normed, w_gate, preferred_element_type=jnp.float32)
    up_pre = jnp.dot(normed, w_up, preferred_element_type=jnp.float32)
    sigmoid_gate = jax.nn.sigmoid(gate_pre)
    activated = gate_pre * sigmoid_gate
    hidden = (activated * up_pre).astype(jnp.bfloat16)
    down_part = (0.5 * outer_sum(cotangent, hidden)).astype(jnp.bfloat16)
    grad_down, early_down = scatter_fs(down_part, True)
    dhidden = jnp.dot(cotangent, w_down, preferred_element_type=jnp.float32)
    dgate = (
        0.5 * dhidden * up_pre * sigmoid_gate * (1.0 + gate_pre * (1.0 - sigmoid_gate))
    ).astype(jnp.bfloat16)
    dupper = (0.5 * dhidden * activated).astype(jnp.bfloat16)
    gate_part = outer_sum(normed, dgate).astype(jnp.bfloat16)
    grad_gate, early_gate = scatter_fs(gate_part, True)
    up_part = outer_sum(normed, dupper).astype(jnp.bfloat16)
    grad_up, early_up = scatter_fs(up_part, False)
    dgate, dupper = lax.optimization_barrier((dgate, dupper, early_down))[:2]
    dnormed = transposed(dgate, w_gate) + transposed(dupper, w_up)
    gain_total = sum_all(jnp.sum(dnormed * unit_rows, axis=0))
    weighted = dnormed * norm_gain.astype(jnp.float32)
    branch = row_scale * (
        weighted - unit_rows * jnp.mean(weighted * unit_rows, axis=1, keepdims=True)
    )
    own_count = earlier_in.shape[0] // lax.axis_size("tp")
    summed = lax.psum_scatter(
        branch.astype(jnp.bfloat16), "tp", scatter_dimension=0, tiled=True
    ).astype(jnp.float32)
    earlier_grad = (own_rows(cotangent, own_count).astype(jnp.float32) + summed).astype(
        jnp.bfloat16
    )
    later_in = lax.optimization_barrier((later_in, early_gate, early_up))[0]
    later_out, later_hidden = forward(later_in, norm_gain, (w_gate, w_up, w_down))
    return (
        later_out,
        later_hidden,
        earlier_grad,
        gate_sum + grad_gate,
        up_sum + grad_up,
        down_sum + grad_down,
        gain_sum + gain_total,
    )


def solution(mesh):
    placed = (
        P("fs", None),
        P("fs", None),
        P("fs", None),
        P("fs", "tp"),
        P("fs", "tp"),
        P("fs", "tp"),
        P(),
        P("fs", "tp"),
        P("fs", "tp"),
        P("fs", "tp"),
        P(),
    )
    return jax.shard_map(
        local,
        mesh=mesh,
        in_specs=placed,
        out_specs=(
            P(("fs", "tp"), None),
            P("fs", "tp"),
            P(("fs", "tp"), None),
            P("fs", "tp"),
            P("fs", "tp"),
            P("fs", "tp"),
            P(),
        ),
        check_vma=False,
    )
```
